32 devices in a mesh: sp: 8 (over z, y), tp: 4 (over x, core).
Axes of the slice: x: 2, y: 2, z: 4, core: 2. Of those that a mesh axis runs over, the one named last changes fastest.
Arguments:
- b_gate: bfloat16 [4096, 2048], P('sp', 'tp'), may hold values from -6 to 6
- c_gate: bfloat16 [4096, 2048], P('sp', 'tp'), may hold values from -6 to 6
- values_in: bfloat16 [4096, 2048], P('sp', 'tp'), may hold values from -6 to 6
- conv_taps: float32 [3, 2048], P(None, 'tp'), may hold values from -4 to 4
- out_proj: bfloat16 [2048, 2048], P('tp'), may hold values from -0.125 to 0.125
- resid: bfloat16 [4096, 2048], P(('sp', 'tp')), may hold values from -6 to 6
- post_gain: float32 [2048], replicated, may hold values from 0.1 to 1.9
- pre_gain: float32 [2048], replicated, may hold values from 0.1 to 1.9
- moe_gain: float32 [2048], replicated, may hold values from 0.1 to 1.9
- routes: int32 [4096, 4], P(('sp', 'tp')), may hold values from 0 to 7, all different within a row; in each aligned block of 128 rows (0 to 127, 128 to 255, ...) at most 128 rows name the same one
- route_weight: float32 [4096, 4], P(('sp', 'tp')), may hold values from 0.1 to 1
- gate_w: bfloat16 [8, 2048, 640], P('sp'), may hold values from -1 to 1
- up_w: bfloat16 [8, 2048, 640], P('sp'), may hold values from -1 to 1
- down_w: bfloat16 [8, 640, 2048], P('sp'), may hold values from -0.25 to 0.25
Outputs:
- result: bfloat16 [4096, 2048], P(('sp', 'tp'))
The draws below stay inside these ranges and needn't reach their ends.
Inputs may be any that keep to these rules, and one draw needn't show every extreme that they name: `routes`: each row names 4 different experts; within each aligned block of 128 rows no expert is named by more than 128 rows.
All inputs are finite; a program needn't handle non-finite values.
Results may differ from the reference program's by a relative error of at most 0.007.
Values may be sent and summed in bfloat16 or wider, within the bound.
A program may use at most 64 MiB of HBM per device.

```python
import math
import jax
import jax.numpy as jnp
import numpy as np
from jax import lax

D = 2048
FF = 640
TOPK = 4
ROWS = 128
TOKENS = 4096
EXPERTS = 8
CAP = 128
N_SP = 8
N_TP = 4


def expert_matrix(key):
    scale = D ** (-0.5)
    sample = jax.random.normal(key, (EXPERTS, D, FF), jnp.float32) * scale
    return jnp.clip(sample, -1.0, 1.0).astype(jnp.bfloat16)


def draw_gate_w(key, part):
    return expert_matrix(jax.random.fold_in(key, 11))


def draw_up_w(key, part):
    return expert_matrix(jax.random.fold_in(key, 23))


def steps_of(stream_key, extent, pieces, low, largest):
    level, own = 1.0, jax.random.fold_in(stream_key, 6)
    for position, blocks in pieces:
        heights = jnp.exp(jax.random.uniform(jax.random.fold_in(own, position), (blocks,), jnp.float32, low / len(pieces), largest / len(pieces)))
        level = level * jnp.repeat(heights, extent[position] // blocks).reshape([-1 if axis == position else 1 for axis in range(len(extent))])
    return level


def deal_out(stream_key, own, number, rows, number_of, top, most, lean):
    ranking = jax.random.permutation(stream_key, number_of)
    crowded, ordinary = shares(number_of, rows * top, most, lean, True), shares(number_of, rows * top, most, lean, False)
    places = jnp.arange(number_of)

    def named(lengths, offset_by):
        used = int((lengths > 0).sum())
        fixed = max(1, used // 4)
        passed = fixed + (places - fixed + offset_by * (used - fixed)) % max(1, number_of - fixed)
        return jnp.zeros((number_of,), jnp.int32).at[ranking[jnp.where(places < fixed, places, passed)]].set(jnp.asarray(lengths, jnp.int32))

    lengths = jnp.where(number % 4 == 0, named(crowded, number // 4), named(ordinary, number - number // 4 - 1))
    mixed = jax.random.permutation(jax.random.fold_in(own, 3), number_of)
    source_of, sink = mixed[0:number_of // 2 * 2:2], mixed[1:number_of // 2 * 2:2]
    margin = jnp.minimum(lengths[source_of] - 1, most - lengths[sink]) // 2
    margin = jnp.where((source_of == ranking[0]) | (sink == ranking[0]) | (lengths[sink] == 0), 0, jnp.maximum(margin, 0))
    passed = jax.random.randint(jax.random.fold_in(own, 4), (number_of // 2,), 0, 1 << 20) % (margin + 1)
    lengths = lengths.at[source_of].add(-passed).at[sink].add(passed)
    labels = jnp.searchsorted(jnp.cumsum(lengths), jnp.arange(rows * top), side="right").astype(jnp.int32)
    listing = labels.reshape(top, rows).T
    listing = listing[jax.random.permutation(jax.random.fold_in(own, 1), rows)]
    offset_by = jax.random.randint(jax.random.fold_in(own, 2), (rows, 1), 0, top)
    return jnp.take_along_axis(listing, (jnp.arange(top)[None, :] + offset_by) % top, axis=1)


def shares(amount, total, most, skew, full):
    portions = [(1 << 20) // math.isqrt(standing ** skew) + 1 for standing in range(1, amount + 1)]
    largest = most if full else min(most, max(-(-total // amount), total * portions[0] // sum(portions)))
    least = 1 if total - largest >= amount - 1 else 0
    holding, surplus = [largest] + [least] * (amount - 1), total - largest - least * (amount - 1)
    while surplus > 0:
        free = [i for i in range(1, amount) if holding[i] < largest] or [i for i in range(1, amount) if holding[i] < most]
        mass, budget = sum([portions[i] for i in free]), surplus
        for i in free:
            more = min(most - holding[i], max(1, budget * portions[i] // mass), surplus)
            holding[i] = holding[i] + more
            surplus = surplus - more
    return np.array(holding)


def bell_draw(key, extent, width, most, cuts=(), kind=jnp.bfloat16):
    drawn = jax.random.normal(key, extent, jnp.float32) * width
    if len(cuts) > 0:
        drawn = steps_of(key, extent, cuts, -0.22, 0.18) * drawn
    return jnp.clip(drawn, min=-most, max=most).astype(kind)


def setup_inputs(seed: int = 0) -> dict:
    arg_keys = jax.random.split(jax.random.key(seed), 15)
    b_gate = bell_draw(arg_keys[0], (TOKENS, D), 1.0, 6.0, ((0, 8), (1, 4)))
    c_gate = bell_draw(arg_keys[1], (TOKENS, D), 1.0, 6.0, ((0, 8), (1, 4)))
    values_in = bell_draw(arg_keys[2], (TOKENS, D), 1.0, 6.0, ((0, 8), (1, 4)))
    conv_taps = bell_draw(arg_keys[3], (3, D), 0.577, 4.0, ((1, 4),), jnp.float32)
    out_proj = bell_draw(arg_keys[4], (D, D), D ** -0.5, 0.125, ((0, 4),))
    resid = bell_draw(arg_keys[5], (TOKENS, D), 1.0, 6.0, ((0, 32),))
    post_gain = jnp.clip(1.0 + 0.18 * jax.random.normal(arg_keys[6], (D,), jnp.float32), 0.1, 1.9)
    pre_gain = jnp.clip(1.0 + 0.18 * jax.random.normal(arg_keys[7], (D,), jnp.float32), 0.1, 1.9)
    moe_gain = jnp.clip(1.0 + 0.18 * jax.random.normal(arg_keys[8], (D,), jnp.float32), 0.1, 1.9)
    routes_keys = jax.random.split(jax.random.fold_in(arg_keys[9], 1), TOKENS // ROWS)
    routes_turns = jax.random.permutation(jax.random.fold_in(arg_keys[9], 3), TOKENS // ROWS)
    routes = jax.vmap(lambda own, number: deal_out(jax.random.fold_in(arg_keys[9], 2), own, number, ROWS, EXPERTS, TOPK, CAP, 1))(routes_keys, routes_turns).reshape((TOKENS, TOPK))
    route_weight = jnp.clip(0.1 + 0.9 * jax.random.uniform(arg_keys[10], (TOKENS, TOPK), jnp.float32) ** steps_of(arg_keys[10], (TOKENS, TOPK), ((0, 32),), -0.2, 0.2), 0.1, 1.0)
    gate_w = draw_gate_w(jax.random.fold_in(arg_keys[14], 71), 0)
    up_w = draw_up_w(jax.random.fold_in(arg_keys[14], 71), 0)
    down_w = bell_draw(arg_keys[13], (EXPERTS, FF, D), FF ** -0.5, 0.25, ((0, 8),))
    return {"b_gate": b_gate, "c_gate": c_gate, "values_in": values_in, "conv_taps": conv_taps, "out_proj": out_proj, "resid": resid, "post_gain": post_gain, "pre_gain": pre_gain, "moe_gain": moe_gain, "routes": routes, "route_weight": route_weight, "gate_w": gate_w, "up_w": up_w, "down_w": down_w}


epsilon = 1e-06

def rms_norm(vector, gain):
    return vector * lax.rsqrt(lax.optimization_barrier(jnp.mean(vector * vector, axis=-1, keepdims=True)) + epsilon) * gain

def reference(b_gate, c_gate, values_in, conv_taps, out_proj, resid, post_gain, pre_gain, moe_gain, routes, route_weight, gate_w, up_w, down_w):
    length = b_gate.shape[0]
    product = c_gate.astype(jnp.float32) * values_in.astype(jnp.float32)
    padded = jnp.pad(product, ((2, 0), (0, 0)))
    filtered = padded[0:length] * conv_taps[0] + padded[1:length + 1] * conv_taps[1] + padded[2:length + 2] * conv_taps[2]
    mixed = (b_gate.astype(jnp.float32) * filtered).astype(jnp.bfloat16)
    projected = jnp.dot(mixed, out_proj, preferred_element_type=jnp.float32)
    stream = (resid.astype(jnp.float32) + rms_norm(projected, post_gain)).astype(jnp.bfloat16)
    normed = rms_norm(stream.astype(jnp.float32), pre_gain).astype(jnp.bfloat16)
    flat_ids = routes.reshape(-1).astype(jnp.int32)
    flat_weight = route_weight.reshape(-1)
    assigned = flat_ids.shape[0]
    order = jnp.argsort(flat_ids, stable=True).astype(jnp.int32)
    counts = jnp.bincount(flat_ids, length=EXPERTS).astype(jnp.int32)
    starts = (jnp.cumsum(counts) - counts).astype(jnp.int32)
    bound = CAP * N_SP * N_TP
    offsets = jnp.arange(bound, dtype=jnp.int32)

    def one_expert(total, expert_id):
        positions = jnp.minimum(starts[expert_id] + offsets, assigned - 1).astype(jnp.int32)
        valid = (offsets < counts[expert_id]).astype(jnp.float32)
        picked = order[positions]
        token_ids = (picked // TOPK).astype(jnp.int32)
        rows_in = normed[token_ids]
        gate_pre = jnp.dot(rows_in, gate_w[expert_id], preferred_element_type=jnp.float32)
        up_pre = jnp.dot(rows_in, up_w[expert_id], preferred_element_type=jnp.float32)
        gate_act = jnp.minimum(gate_pre, 7.0)
        up_act = jnp.clip(up_pre, -7.0, 7.0)
        hidden = (gate_act * jax.nn.sigmoid(1.702 * gate_act) * (up_act + 1.0)).astype(jnp.bfloat16)
        expert_out = jnp.dot(hidden, down_w[expert_id], preferred_element_type=jnp.float32).astype(jnp.bfloat16)
        scaled = expert_out.astype(jnp.float32) * (flat_weight[picked] * valid)[:, None]
        return (total.at[token_ids].add(scaled), None)
    combined, _ = lax.scan(one_expert, jnp.zeros((length, D), jnp.float32), jnp.arange(EXPERTS, dtype=jnp.int32))
    return (stream.astype(jnp.float32) + rms_norm(combined, moe_gain)).astype(jnp.bfloat16)
```

```python
import functools

import jax
import jax.numpy as jnp
from jax import lax
from jax.experimental import pallas as pl
from jax.experimental.pallas import tpu as pltpu
from jax.sharding import PartitionSpec as P

epsilon = 1e-06


def shifted(shard, axis, by):
    devices = lax.axis_size(axis)
    pairs = [(i, i + by) for i in range(devices) if 0 <= i + by < devices]
    return lax.ppermute(shard, axis, pairs)


def rms_norm(vector, gain):
    return vector * lax.rsqrt(jnp.mean(vector * vector, axis=-1, keepdims=True) + epsilon) * gain


def expert_rows(rows_in, gate_w, up_w, down_w):
    gate_pre = jnp.dot(rows_in, gate_w[0], preferred_element_type=jnp.float32)
    up_pre = jnp.dot(rows_in, up_w[0], preferred_element_type=jnp.float32)
    gate_act = jnp.minimum(gate_pre, 7.0)
    up_act = jnp.clip(up_pre, -7.0, 7.0)
    hidden = (gate_act * jax.nn.sigmoid(1.702 * gate_act) * (up_act + 1.0)).astype(jnp.bfloat16)
    return jnp.dot(hidden, down_w[0], preferred_element_type=jnp.float32).astype(jnp.bfloat16)


def by_slot(normed, routes, route_weight, gate_w, up_w, down_w):
    own_count = normed.shape[0]
    width = normed.shape[1]
    top_count = routes.shape[1]
    experts = lax.axis_size("sp")
    capacity = 2 * own_count * top_count // experts
    flat_ids = routes.reshape(-1)
    assigned = flat_ids.shape[0]
    onehot = (flat_ids[:, None] == jnp.arange(experts, dtype=jnp.int32)[None, :]).astype(jnp.int32)
    earlier = jnp.cumsum(onehot, axis=0) - onehot
    slot_index = jnp.sum(earlier * onehot, axis=1)
    target = flat_ids * capacity + slot_index
    source = (
        jnp.full((experts * capacity,), assigned, jnp.int32)
        .at[target]
        .set(jnp.arange(assigned, dtype=jnp.int32))
    )
    row_index = jnp.where(source < assigned, source // top_count, own_count)
    with_blank = jnp.concatenate([normed, jnp.zeros((1, width), jnp.bfloat16)], axis=0)
    outgoing = with_blank[row_index].reshape(experts, capacity, width)
    slots_in = lax.all_to_all(outgoing, "sp", split_axis=0, concat_axis=0, tiled=True)
    expert_out = expert_rows(slots_in, gate_w, up_w, down_w)
    returned = lax.all_to_all(expert_out, "sp", split_axis=0, concat_axis=0, tiled=True)
    chosen = returned.reshape(experts * capacity, width)[target].astype(jnp.float32)
    weighted = chosen * route_weight.reshape(-1)[:, None]
    combined = jnp.sum(weighted.reshape(own_count, top_count, width), axis=1)
    return combined


def copy_to(axis, device, src, dst, send_sem, recv_sem):
    return pltpu.make_async_remote_copy(
        src_ref=src,
        dst_ref=dst,
        send_sem=send_sem,
        recv_sem=recv_sem,
        device_id={axis: device},
        device_id_type=pl.DeviceIdType.MESH,
    )


def greet_all(axis, n):
    me = lax.axis_index(axis)
    barrier = pltpu.get_barrier_semaphore()
    for step in range(1, n):
        pl.semaphore_signal(
            barrier,
            inc=1,
            device_id={axis: lax.rem(me + step, n)},
            device_id_type=pl.DeviceIdType.MESH,
        )
    pl.semaphore_wait(barrier, n - 1)


def on_line(place, length):
    return jnp.logical_and(place >= 0, place < length)


def gather_kernel(axis, n, early, own, spread, out, weights, *sems):
    own_sem, pair_s, pair_r, line_s, line_r, both_s, both_r, w_s, w_r = sems
    length = n // 2
    me = lax.axis_index(axis)
    place, side = me // 2, lax.rem(me, 2)
    mate = place * 2 + 1 - side
    rows = own.shape[0]
    head, tail = pl.ds(0, early), pl.ds(early, rows - early)
    greet_all(axis, n)

    def pair_copy(origin, k, part, src=None):
        slot = out.at[origin * 2 + side, part]
        return copy_to(axis, mate, slot if src is None else src, slot, pair_s.at[k], pair_r.at[k])

    def line_copy(origin, way, k, sem, src=None):
        slot = out.at[origin * 2 + side, tail]
        return copy_to(
            axis,
            lax.rem(place + way + length, length) * 2 + side,
            slot if src is None else src,
            slot,
            line_s.at[k, sem],
            line_r.at[k, sem],
        )

    def both_copy(origin, member, way, k, sem):
        slot = out.at[origin * 2 + member, head]
        return copy_to(
            axis,
            lax.rem(place + way + length, length) * 2 + side,
            slot,
            slot,
            both_s.at[k, sem, member],
            both_r.at[k, sem, member],
        )

    ways = ((1, 0), (-1, 1))
    here = pltpu.make_async_copy(own, out.at[me], own_sem)
    here.start()
    swap = pair_copy(place, 2 * length, head, own.at[head])
    swap.start()
    for way, sem in ways:
        @pl.when(on_line(place + way, length))
        def _():
            line_copy(place, way, 0, sem, own.at[tail]).start()
    pair_copy(place, 0, tail, own.at[tail]).start()
    for step in range(1, n):
        expert = lax.rem(me + step, n)
        copy_to(axis, expert, spread.at[expert], weights.at[me], w_s.at[step], w_r.at[step]).start()
    weights[me] = spread[me]
    here.wait()
    swap.wait_recv()
    for way, sem in ways:
        @pl.when(on_line(place + way, length))
        def _():
            for member in range(2):
                both_copy(place, member, way, 0, sem).start()
    for k in range(1, length):
        for way, sem in ways:
            origin = place - way * k
            @pl.when(on_line(origin, length))
            def _():
                line_copy(origin, way, k - 1, sem).wait_recv()

                @pl.when(on_line(place + way, length))
                def _():
                    line_copy(origin, way, k, sem).start()
                pair_copy(origin, 2 * k - sem, tail).start()
        for way, sem in ways:
            origin = place - way * k
            @pl.when(on_line(origin, length))
            def _():
                for member in range(2):
                    both_copy(origin, member, way, k - 1, sem).wait_recv()

                    @pl.when(on_line(place + way, length))
                    def _():
                        both_copy(origin, member, way, k, sem).start()
    swap.wait_send()
    pair_copy(place, 0, tail).wait()
    for step in range(1, n):
        expert = lax.rem(me + step, n)
        copy_to(axis, expert, spread.at[expert], weights.at[me], w_s.at[step], w_r.at[step]).wait()
    for k in range(length):
        for way, sem in ways:
            origin = place - way * k
            @pl.when(on_line(origin, length))
            def _():
                if k > 0:
                    pair_copy(origin, 2 * k - sem, tail).wait()

                @pl.when(on_line(place + way, length))
                def _():
                    line_copy(origin, way, k, sem).wait_send()
                    for member in range(2):
                        both_copy(origin, member, way, k, sem).wait_send()


def gather_rows(axis, own, spread, collective_id):
    n = lax.axis_size(axis)
    rows, width = own.shape
    length = n // 2
    early = rows * 3 // 8 // 16 * 16
    vmem = pl.BlockSpec(memory_space=pltpu.VMEM)
    dma = pltpu.SemaphoreType.DMA
    return pl.pallas_call(
        functools.partial(gather_kernel, axis, n, early),
        out_shape=(
            jax.ShapeDtypeStruct((n, rows, width), own.dtype),
            jax.ShapeDtypeStruct((n, 1, rows), spread.dtype),
        ),
        in_specs=[vmem, vmem],
        out_specs=(vmem, vmem),
        scratch_shapes=[
            dma,
            dma((2 * length + 1,)),
            dma((2 * length + 1,)),
            dma((length, 2)),
            dma((length, 2)),
            dma((length, 2, 2)),
            dma((length, 2, 2)),
            dma((n,)),
            dma((n,)),
        ],
        compiler_params=pltpu.CompilerParams(collective_id=collective_id, has_side_effects=True),
    )(own, spread)


def reduce_kernel(axis, n, early, part, out, *scratch):
    pair_in, line_in, line_out, swap_in, swap_out, both_in, both_out = scratch[:7]
    pair_s, pair_r, line_s, line_r, both_s, both_r, swap_s, swap_r = scratch[7:]
    length = n // 2
    me = lax.axis_index(axis)
    place, side = me // 2, lax.rem(me, 2)
    mate = place * 2 + 1 - side
    rows = part.shape[1]
    head, tail = pl.ds(0, early), pl.ds(early, rows - early)
    ways = ((1, 0), (-1, 1))
    f32 = jnp.float32
    greet_all(axis, n)

    def pair_copy(target, k):
        return copy_to(
            axis, mate, part.at[target * 2 + 1 - side, tail], pair_in.at[k], pair_s.at[k], pair_r.at[k]
        )

    def line_copy(way, k, sem):
        return copy_to(
            axis,
            lax.rem(place + way + length, length) * 2 + side,
            line_out.at[k, sem],
            line_in.at[k - 1, sem],
            line_s.at[k, sem],
            line_r.at[k - 1, sem],
        )

    def line_arrival(way, k, sem):
        return copy_to(
            axis,
            lax.rem(place - way + length, length) * 2 + side,
            line_out.at[k, sem],
            line_in.at[k, sem],
            line_s.at[k, sem],
            line_r.at[k, sem],
        )

    def both_copy(way, k, sem, member):
        return copy_to(
            axis,
            lax.rem(place + way + length, length) * 2 + side,
            both_out.at[k, sem, member],
            both_in.at[k - 1, sem, member],
            both_s.at[k, sem, member],
            both_r.at[k - 1, sem, member],
        )

    def both_arrival(way, k, sem, member):
        return copy_to(
            axis,
            lax.rem(place - way + length, length) * 2 + side,
            both_out.at[k, sem, member],
            both_in.at[k, sem, member],
            both_s.at[k, sem, member],
            both_r.at[k, sem, member],
        )

    def slot_of(k, sem):
        return 2 * k - sem if k else 0

    for k in range(length - 1, -1, -1):
        for way, sem in ways[: 2 if k else 1]:
            target = place + way * k
            @pl.when(on_line(target, length))
            def _():
                pair_copy(target, slot_of(k, sem)).start()
    for k in range(length - 1, 0, -1):
        for way, sem in ways if early else ():
            target = place + way * k
            @pl.when(on_line(target, length))
            def _():
                for member in range(2):
                    both_out[k, sem, member] = part[target * 2 + member, head]

                    @pl.when(on_line(place - way, length))
                    def _():
                        both_arrival(way, k, sem, member).wait_recv()
                        total = part[target * 2 + member, head].astype(f32)
                        total = total + both_in[k, sem, member].astype(f32)
                        both_out[k, sem, member] = total.astype(part.dtype)
                    both_copy(way, k, sem, member).start()
        for way, sem in ways:
            target = place + way * k
            @pl.when(on_line(target, length))
            def _():
                slot = slot_of(k, sem)
                pair_copy(target, slot).wait_recv()
                total = part[target * 2 + side, tail].astype(f32) + pair_in[slot].astype(f32)

                @pl.when(jnp.logical_not(on_line(place - way, length)))
                def _():
                    line_out[k, sem] = total.astype(part.dtype)

                @pl.when(on_line(place - way, length))
                def _():
                    line_arrival(way, k, sem).wait_recv()
                    more = total + line_in[k, sem].astype(f32)
                    line_out[k, sem] = more.astype(part.dtype)
                line_copy(way, k, sem).start()
    if early:
        for member in range(2):
            swap_out[member] = part[place * 2 + member, head].astype(f32)
            for way, sem in ways:
                @pl.when(on_line(place - way, length))
                def _():
                    both_arrival(way, 0, sem, member).wait_recv()
                    swap_out[member] += both_in[0, sem, member].astype(f32)
        swap_in[0] = swap_out[1 - side].astype(part.dtype)
        swap = copy_to(axis, mate, swap_in.at[0], swap_in.at[1], swap_s, swap_r)
        swap.start()
    pair_copy(place, 0).wait_recv()
    out[tail] = part[place * 2 + side, tail].astype(f32) + pair_in[0].astype(f32)
    for way, sem in ways:
        @pl.when(on_line(place - way, length))
        def _():
            line_arrival(way, 0, sem).wait_recv()
            out[tail] += line_in[0, sem].astype(f32)
    if early:
        swap.wait()
        out[head] = swap_out[side] + swap_in[1].astype(f32)
    for k in range(length - 1, -1, -1):
        for way, sem in ways[: 2 if k else 1]:
            target = place + way * k
            @pl.when(on_line(target, length))
            def _():
                pair_copy(target, slot_of(k, sem)).wait_send()
                if k:
                    line_copy(way, k, sem).wait_send()
                    if early:
                        for member in range(2):
                            both_copy(way, k, sem, member).wait_send()


def reduce_rows(axis, part, early, collective_id):
    n, rows, width = part.shape
    length = n // 2
    late = rows - early
    vmem = pl.BlockSpec(memory_space=pltpu.VMEM)
    dma = pltpu.SemaphoreType.DMA
    first = max(early, 16)
    return pl.pallas_call(
        functools.partial(reduce_kernel, axis, n, early),
        out_shape=jax.ShapeDtypeStruct((rows, width), jnp.float32),
        in_specs=[vmem],
        out_specs=vmem,
        scratch_shapes=[
            pltpu.VMEM((2 * length, late, width), part.dtype),
            pltpu.VMEM((length, 2, late, width), part.dtype),
            pltpu.VMEM((length, 2, late, width), part.dtype),
            pltpu.VMEM((2, first, width), part.dtype),
            pltpu.VMEM((2, first, width), jnp.float32),
            pltpu.VMEM((length, 2, 2, first, width), part.dtype),
            pltpu.VMEM((length, 2, 2, first, width), part.dtype),
            dma((2 * length,)),
            dma((2 * length,)),
            dma((length, 2)),
            dma((length, 2)),
            dma((length, 2, 2)),
            dma((length, 2, 2)),
            dma,
            dma,
        ],
        compiler_params=pltpu.CompilerParams(collective_id=collective_id, has_side_effects=True),
    )(part)


def every_row(normed, routes, route_weight, gate_w, up_w, down_w):
    experts = lax.axis_size("sp")
    rows, width = normed.shape
    named = routes[:, :, None] == jnp.arange(experts, dtype=jnp.int32)[None, None, :]
    spread = jnp.sum(jnp.where(named, route_weight[:, :, None], 0.0), axis=1)
    gathered, weights = gather_rows("sp", normed, spread.T[:, None, :], 1)
    rows_in = gathered.reshape(experts * rows, width)
    expert_out = expert_rows(rows_in, gate_w, up_w, down_w)
    weighted = expert_out.astype(jnp.float32) * weights.reshape(experts * rows)[:, None]
    part = weighted.astype(jnp.bfloat16).reshape(experts, rows, width)
    return reduce_rows("sp", part, rows * 3 // 8 // 16 * 16, 2)


def expert_kernel(n, t_n, cross, own, spread, gate, up, down, out, *scratch):
    x_buf, w_in, w_out, hid, hid_out, part, red_in, red_out, w_row, w_col = scratch[:10]
    (load_s, w_s, w_r, zt_s, zt_r, zh_s, zh_r, yt_s, yt_r, yh_s, yh_r,
     h_s, h_r, red_s, red_r, dy_s, dy_r, dt_s, dt_r, dm_s, dm_r) = scratch[10:]
    length = n // 2
    f32, bf16 = jnp.float32, jnp.bfloat16
    me = lax.axis_index("sp")
    p, side = me // 2, lax.rem(me, 2)
    mate = p * 2 + 1 - side
    rows, width = own.shape
    half = rows // 2
    keep = half - cross
    hidden = gate.shape[2]
    lanes = 128
    tiles = hidden // lanes
    t_me = lax.axis_index("tp")
    core = lax.rem(t_me, 2)
    t_mate = t_me + 1 - 2 * core
    share = hidden // t_n
    last = length - 1
    ways = ((0, 1), (1, -1))

    loads = []
    for j in range(tiles):
        for m, src in enumerate((gate, up)):
            loads.append(pltpu.make_async_copy(
                src.at[0, :, pl.ds(j * lanes, lanes)],
                w_in.at[:, pl.ds((2 * j + m) * lanes, lanes)],
                load_s.at[2 * j + m]))
    loads.append(pltpu.make_async_copy(down.at[0], w_out.at[pl.ds(0, hidden)], load_s.at[2 * tiles]))
    for load in loads:
        load.start()
    place_own = pltpu.make_async_copy(own, x_buf.at[p, side], load_s.at[2 * tiles + 1])
    place_own.start()
    barrier = pltpu.get_barrier_semaphore()
    for axis, count in (("sp", n), ("tp", t_n)):
        here = lax.axis_index(axis)
        for step in range(1, count):
            pl.semaphore_signal(
                barrier,
                inc=1,
                device_id={axis: lax.rem(here + step, count)},
                device_id_type=pl.DeviceIdType.MESH,
            )
    pl.semaphore_wait(barrier, n + t_n - 2)

    def down_slot(t):
        return w_out.at[pl.ds(hidden + t * share, share)]

    down_y = copy_to("sp", mate, down.at[0, pl.ds(t_me * share, share)], down_slot(t_me), dy_s, dy_r)

    def down_x(step):
        there = lax.rem(t_me + 2 * step, t_n)
        return copy_to("tp", there, down_slot(t_me), down_slot(t_me), dt_s.at[step], dt_r.at[step])

    def down_mate(step):
        origin = lax.rem(t_me + t_n - 2 * step, t_n)
        return copy_to("tp", t_mate, down_slot(origin), down_slot(origin), dm_s.at[step], dm_r.at[step])

    def weight_copy(step):
        expert = lax.rem(me + step, n)
        return copy_to("sp", expert, spread.at[expert], w_row.at[me], w_s.at[step], w_r.at[step])

    def at_rows(c, first, count):
        return pl.ds(pl.multiple_of(c * half + first, 16), count)

    def z_copies(o, c, d):
        there = (p + ways[d][1] + length) % length * 2 + side
        tail = x_buf.at[o, side, at_rows(c, 0, keep)]
        copies = [copy_to("sp", there, tail, tail, zt_s.at[c, o, d], zt_r.at[c, o, d])]
        if cross:
            head = x_buf.at[o, :, at_rows(c, keep, cross)]
            copies.append(copy_to("sp", there, head, head, zh_s.at[c, o, d], zh_r.at[c, o, d]))
        return copies

    def y_copy(o, c):
        tail = x_buf.at[o, side, at_rows(c, 0, keep)]
        return copy_to("sp", mate, tail, tail, yt_s.at[c, o], yt_r.at[c, o])

    def swap_copy(c):
        head = x_buf.at[p, side, at_rows(c, keep, cross)]
        return copy_to("sp", mate, head, head, yh_s.at[c], yh_r.at[c])

    def hidden_copy(o, c):
        r = at_rows(c, 0, half)
        return copy_to(
            "sp", mate, hid_out.at[o, r], hid.at[o, r, pl.ds(hidden, hidden)], h_s.at[c, o], h_r.at[c, o]
        )

    def sum_copy(t, c, d):
        r = at_rows(c, 0, half)
        there = (p + ways[d][1] + length) % length * 2 + side
        return copy_to(
            "sp", there, red_out.at[t, r], red_in.at[t, d, r], red_s.at[c, t], red_r.at[c, t, d]
        )

    def behind(d):
        return p if d == 0 else last - p

    def arrival(d, j):
        count = behind(d)
        c = jnp.where(j > count, 1, 0)
        far = jnp.where(j > count, 2 * count + 1 - j, j)
        o = jnp.clip(p - ways[d][1] * far, 0, last)
        return jnp.logical_and(j >= 1, j <= 2 * count), o, c

    def ahead(d):
        return on_line(p + ways[d][1], length)

    def send_on(o, c, d):
        @pl.when(ahead(d))
        def _():
            for copy in z_copies(o, c, d):
                copy.start()

    def gate_up(o, c):
        r = at_rows(c, 0, half)
        weight = w_col[pl.ds(o * 2, 2), r, :].reshape(2 * half, lanes)

        def tile(j, carry):
            rows_in = x_buf[o, :, r, :].reshape(2 * half, width)
            both = jnp.dot(rows_in, w_in[:, pl.ds(pl.multiple_of(j * 2 * lanes, 2 * lanes), 2 * lanes)],
                           preferred_element_type=f32)
            gate_act = jnp.minimum(both[:, :lanes], 7.0)
            up_act = jnp.clip(both[:, lanes:], -7.0, 7.0)
            value = gate_act * jax.nn.sigmoid(1.702 * gate_act) * (up_act + 1.0) * weight
            mine = side == 0
            col = pl.ds(pl.multiple_of(j * lanes, lanes), lanes)
            hid[o, r, col] = jnp.where(mine, value[:half], value[half:]).astype(bf16)
            hid_out[o, r, col] = jnp.where(mine, value[half:], value[:half]).astype(bf16)
            return carry

        lax.fori_loop(0, tiles, tile, 0)
        hidden_copy(o, c).start()

    def down_rows(o, c):
        hidden_copy(o, c).wait_recv()
        r = at_rows(c, 0, half)
        step = 2 * lanes

        def tile(j, carry):
            col = pl.ds(pl.multiple_of(j * step, step), step)
            part[o, r, col] = jnp.dot(hid[o, r, :], w_out[:, col], preferred_element_type=f32)
            return carry

        lax.fori_loop(0, width // step, tile, 0)

    def flow(t, c, d, valid):
        r = at_rows(c, 0, half)
        t = jnp.clip(t, 0, last)
        final = t == p
        incoming = on_line(p - ways[d][1], length)

        @pl.when(jnp.logical_and(valid, incoming))
        def _():
            sum_copy(t, c, d).wait_recv()
            part[t, r, :] += red_in[t, d, r, :].astype(f32)

        @pl.when(jnp.logical_and(valid, jnp.logical_not(final)))
        def _():
            red_out[t, r, :] = part[t, r, :].astype(bf16)
            sum_copy(t, c, d).start()

    place_own.wait()
    for c in range(2):
        if cross:
            swap_copy(c).start()
    for d in range(2):
        @pl.when(ahead(d))
        def _():
            z_copies(p, 0, d)[0].start()
    y_copy(p, 0).start()
    down_y.start()
    for step in range(1, n):
        weight_copy(step).start()
    w_row[me] = spread[me]
    if cross:
        swap_copy(0).wait_recv()
    for d in range(2):
        @pl.when(ahead(d))
        def _():
            for copy in z_copies(p, 0, d)[1:]:
                copy.start()
    for step in range(1, n):
        weight_copy(step).wait_recv()
    for k in range(n):
        w_col[k] = jnp.broadcast_to(w_row[k, 0, :][None, :], (lanes, rows)).T
    for load in loads:
        load.wait()
    if cross:
        swap_copy(1).wait_recv()
    for d in range(2):
        @pl.when(behind(d) == 0)
        def _():
            send_on(p, 1, d)
    down_y.wait_recv()
    for step in range(1, t_n // 2):
        down_x(step).start()
    for step in range(t_n // 2):
        if step:
            down_x(step).wait_recv()
        down_mate(step).start()
    for step in range(t_n // 2):
        down_mate(step).wait_recv()

    own_slot = length + 1

    def slot(i, carry):
        for d in range(2):
            there, o, c = arrival(d, i + 1)

            @pl.when(there)
            def _():
                for copy in z_copies(o, c, d):
                    copy.wait_recv()
                send_on(o, c, d)
                y_copy(o, c).start()

            @pl.when(jnp.logical_and(i + 1 == 2 * behind(d), behind(d) > 0))
            def _():
                send_on(p, 1, d)

        @pl.when(i + 1 == own_slot)
        def _():
            y_copy(p, 1).start()

        for d in range(2):
            there, o, c = arrival(d, i)

            @pl.when(there)
            def _():
                y_copy(o, c).wait_recv()
                gate_up(o, c)

        own_now = jnp.logical_or(i == 0, i == own_slot)
        own_c = jnp.where(i == 0, 0, 1)

        @pl.when(own_now)
        def _():
            y_copy(p, own_c).wait_recv()
            gate_up(p, own_c)

        for d in range(2):
            there, o, c = arrival(d, i - 1)

            @pl.when(there)
            def _():
                down_rows(o, c)

        own_then = jnp.logical_or(i == 1, i == own_slot + 1)
        then_c = jnp.where(i == 1, 0, 1)

        @pl.when(own_then)
        def _():
            down_rows(p, then_c)

        f = i - 1
        for d in range(2):
            q = behind(d)
            for c in range(2):
                reach = f - q if c == 0 else 2 * length - 1 - f + q
                valid = jnp.logical_and(jnp.logical_and(reach >= q, reach <= last), f >= 0)
                t = reach if d == 0 else last - reach
                flow(t, c, d, valid)
        return carry

    lax.fori_loop(0, 2 * length + 1, slot, 0)
    out[...] = part[p]

    down_y.wait_send()
    for step in range(t_n // 2):
        if step:
            down_x(step).wait_send()
        down_mate(step).wait_send()
    for step in range(1, n):
        weight_copy(step).wait_send()
    for c in range(2):
        if cross:
            swap_copy(c).wait_send()
        for o in range(length):
            y_copy(o, c).wait_send()
            hidden_copy(o, c).wait_send()

            @pl.when(o != p)
            def _():
                sum_copy(o, c, 0).wait_send()

            for d in range(2):
                passes = o <= p if d == 0 else o >= p

                @pl.when(jnp.logical_and(passes, ahead(d)))
                def _():
                    for copy in z_copies(o, c, d):
                        copy.wait_send()


def fits_line(normed, gate_w):
    n, t_n = lax.axis_size("sp"), lax.axis_size("tp")
    rows, width = normed.shape
    hidden = gate_w.shape[2]
    return (n % 2 == 0 and t_n % 2 == 0 and rows % 128 == 0 and rows == 128
            and width % 256 == 0 and hidden % 128 == 0 and hidden % (16 * t_n) == 0)


def expert_layer(normed, routes, route_weight, gate_w, up_w, down_w):
    n, t_n = lax.axis_size("sp"), lax.axis_size("tp")
    rows, width = normed.shape
    hidden = gate_w.shape[2]
    length = n // 2
    named = routes[:, :, None] == jnp.arange(n, dtype=jnp.int32)[None, None, :]
    spread = jnp.sum(jnp.where(named, route_weight[:, :, None], 0.0), axis=1).T[:, None, :]
    vmem = pl.BlockSpec(memory_space=pltpu.VMEM)
    hbm = pl.BlockSpec(memory_space=pl.ANY)
    dma = pltpu.SemaphoreType.DMA
    bf16 = jnp.bfloat16
    return pl.pallas_call(
        functools.partial(expert_kernel, n, t_n, 16),
        out_shape=jax.ShapeDtypeStruct((rows, width), jnp.float32),
        in_specs=[vmem, vmem, hbm, hbm, hbm],
        out_specs=vmem,
        scratch_shapes=[
            pltpu.VMEM((length, 2, rows, width), bf16),
            pltpu.VMEM((width, 2 * hidden), bf16),
            pltpu.VMEM((2 * hidden, width), bf16),
            pltpu.VMEM((length, rows, 2 * hidden), bf16),
            pltpu.VMEM((length, rows, hidden), bf16),
            pltpu.VMEM((length, rows, width), jnp.float32),
            pltpu.VMEM((length, 2, rows, width), bf16),
            pltpu.VMEM((length, rows, width), bf16),
            pltpu.VMEM((n, 1, rows), jnp.float32),
            pltpu.VMEM((n, rows, 128), jnp.float32),
            dma((2 * (hidden // 128) + 2,)),
            dma((n,)), dma((n,)),
            dma((2, length, 2)), dma((2, length, 2)),
            dma((2, length, 2)), dma((2, length, 2)),
            dma((2, length)), dma((2, length)),
            dma((2,)), dma((2,)),
            dma((2, length)), dma((2, length)),
            dma((2, length)), dma((2, length, 2)),
            dma, dma,
            dma((t_n,)), dma((t_n,)),
            dma((t_n,)), dma((t_n,)),
        ],
        compiler_params=pltpu.CompilerParams(collective_id=1, has_side_effects=True),
    )(normed, spread, gate_w, up_w, down_w)


def body(
    b_gate,
    c_gate,
    values_in,
    conv_taps,
    out_proj,
    resid,
    post_gain,
    pre_gain,
    moe_gain,
    routes,
    route_weight,
    gate_w,
    up_w,
    down_w,
):
    tok_rows = b_gate.shape[0]
    product = c_gate.astype(jnp.float32) * values_in.astype(jnp.float32)
    prior_rows = shifted(product[tok_rows - 2 :], "sp", 1)
    padded = jnp.concatenate([prior_rows, product], axis=0)
    filtered = (
        padded[0:tok_rows] * conv_taps[0]
        + padded[1 : tok_rows + 1] * conv_taps[1]
        + padded[2 : tok_rows + 2] * conv_taps[2]
    )
    mixed_rows = (b_gate.astype(jnp.float32) * filtered).astype(jnp.bfloat16)
    experts = lax.axis_size("sp")
    own_count = resid.shape[0]
    whole_rows = 2 * own_count * routes.shape[1] // experts >= own_count
    share = jnp.dot(mixed_rows, out_proj, preferred_element_type=jnp.float32)
    if whole_rows:
        blocks = share.astype(jnp.bfloat16).reshape(-1, own_count, share.shape[1])
        projected = reduce_rows("tp", blocks, 0, 3)
    else:
        projected = lax.psum_scatter(share, "tp", scatter_dimension=0, tiled=True)
    stream = (resid.astype(jnp.float32) + rms_norm(projected, post_gain)).astype(jnp.bfloat16)
    normed = rms_norm(stream.astype(jnp.float32), pre_gain).astype(jnp.bfloat16)
    if whole_rows:
        mix = expert_layer if fits_line(normed, gate_w) else every_row
    else:
        mix = by_slot
    combined = mix(normed, routes, route_weight, gate_w, up_w, down_w)
    return (stream.astype(jnp.float32) + rms_norm(combined, moe_gain)).astype(jnp.bfloat16)


def solution(mesh):
    placed = (
        P("sp", "tp"),
        P("sp", "tp"),
        P("sp", "tp"),
        P(None, "tp"),
        P("tp", None),
        P(("sp", "tp"), None),
        P(),
        P(),
        P(),
        P(("sp", "tp"), None),
        P(("sp", "tp"), None),
        P("sp", None, None),
        P("sp", None, None),
        P("sp", None, None),
    )
    return jax.shard_map(
        body, mesh=mesh, in_specs=placed, out_specs=P(("sp", "tp"), None), check_vma=False
    )
```
